32 devices in a mesh: sp: 8 (over z, y), tp: 4 (over x, core).
Axes of the slice: x: 2, y: 2, z: 4, core: 2. Of those that a mesh axis runs over, the one named last changes fastest.
Arguments:
- frames: bfloat16 [4, 1024, 1024], P('tp', 'sp'), may hold values from -22 to 22
- norm_gain: float32 [1024], replicated, may hold values from 0.5 to 1.5
- conv_value_w: bfloat16 [1024, 512], P(None, 'tp'), may hold values from -0.1875 to 0.1875
- conv_gate_w: bfloat16 [1024, 512], P(None, 'tp'), may hold values from -0.1875 to 0.1875
- conv_taps: bfloat16 [31, 512], P(None, 'tp'), may hold values from -1 to 1
- conv_bias: float32 [512], P('tp'), may hold values from -1.2 to 1.2
- channel_gain: float32 [512], P('tp'), may hold values from 0.5 to 1.5
- channel_shift: float32 [512], P('tp'), may hold values from -1.2 to 1.2
- query_w: bfloat16 [1024, 1024], P(None, 'tp'), may hold values from -0.1875 to 0.1875
- forget_w: bfloat16 [1024, 1024], P(None, 'tp'), may hold values from -0.1875 to 0.1875
- input_w: bfloat16 [1024, 1024], P(None, 'tp'), may hold values from -0.1875 to 0.1875
- gate_w: bfloat16 [1024, 1024], P(None, 'tp'), may hold values from -0.1875 to 0.1875
- memory_rate: float32 [1024], P('tp'), may hold values from 0.5 to 32
- head_gain: float32 [1024], P('tp'), may hold values from 0.5 to 1.5
- conv_out_w: bfloat16 [512, 1024], P('tp'), may hold values from -0.1875 to 0.1875
- rec_out_w: bfloat16 [1024, 1024], P('tp'), may hold values from -0.125 to 0.125
Outputs:
- mixed: bfloat16 [4, 1024, 1024], P('tp', 'sp')
The draws below stay inside these ranges and needn't reach their ends.
All inputs are finite; a program needn't handle non-finite values.
Results may differ from the reference program's by a relative error of at most 0.015.
The reference program's roundings to bfloat16 on the way (of `normed`, `gated_conv`, `conv_out`, `scores`, `carried_low` and `rec_out`) count: a program that leaves them out, or rounds other values in their place, can miss the bound.
Values may be sent and summed in bfloat16 or wider, within the bound.
A program may use at most 64 MiB of HBM per device.

```python
import math
import jax
import jax.numpy as jnp
from jax import lax

D = 1024
D_CONV = 512
CONV_WIDTH = 31
HEADS = 8
HEAD = 128
D_HG = 1024
POS_DEV = 128
SEQS = 4
SEQ_LEN = 1024
N_SP = 8


def draw_frames(key, part):
    noise_key = jax.random.fold_in(key, 11)
    direction_key = jax.random.fold_in(key, 12)
    level_key = jax.random.fold_in(key, 13)
    block_count = SEQ_LEN // POS_DEV
    noise = jnp.clip(jax.random.normal(noise_key, (SEQS, SEQ_LEN, D), jnp.float32), -6.0, 6.0)
    direction = jnp.clip(jax.random.normal(direction_key, (D,), jnp.float32), -4.0, 4.0)
    levels = jax.random.uniform(level_key, (SEQS, block_count, 1, 1), jnp.float32, -4.0, 4.0)
    spread_levels = jnp.broadcast_to(levels, (SEQS, block_count, POS_DEV, 1)).reshape(SEQS, SEQ_LEN, 1)
    return (noise + spread_levels * direction).astype(jnp.bfloat16)


def shard_levels(stream_key, extent, pieces, low, largest):
    def one(dim, blocks):
        draws = jax.random.uniform(jax.random.fold_in(jax.random.fold_in(stream_key, 6), dim), (blocks,), jnp.float32, low / len(pieces), largest / len(pieces))
        return jnp.repeat(jnp.exp(draws), extent[dim] // blocks).reshape((-1,) + (1,) * (len(extent) - dim - 1))

    gain = one(*pieces[0])
    for cut in pieces[1:]:
        gain = gain * one(*cut)
    return gain


def bell_draw(key, dims, deviation, most, shards=(), held_as=jnp.bfloat16):
    values = deviation * jax.random.normal(key, dims, jnp.float32)
    if shards:
        values = values * shard_levels(key, dims, shards, -0.22, 0.18)
    return jnp.clip(values, -most, most).astype(held_as)


def setup_inputs(seed: int = 0) -> dict:
    arg_keys = jax.random.split(jax.random.key(seed), 17)
    return {
        "frames": draw_frames(jax.random.fold_in(arg_keys[16], 71), 0),
        "norm_gain": jnp.clip(1.0 + 0.1 * jax.random.normal(arg_keys[1], (D,), jnp.float32), 0.5, 1.5),
        "conv_value_w": bell_draw(arg_keys[2], (D, D_CONV), D ** -0.5, 0.1875, ((1, 4),)),
        "conv_gate_w": bell_draw(arg_keys[3], (D, D_CONV), D ** -0.5, 0.1875, ((1, 4),)),
        "conv_taps": bell_draw(arg_keys[4], (CONV_WIDTH, D_CONV), CONV_WIDTH ** -0.5, 1.0, ((1, 4),)),
        "conv_bias": bell_draw(arg_keys[5], (D_CONV,), 0.2, 1.2, ((0, 4),), jnp.float32),
        "channel_gain": jnp.clip(1.0 + 0.1 * jax.random.normal(arg_keys[6], (D_CONV,), jnp.float32), 0.5, 1.5),
        "channel_shift": bell_draw(arg_keys[7], (D_CONV,), 0.2, 1.2, ((0, 4),), jnp.float32),
        "query_w": bell_draw(arg_keys[8], (D, D_HG), D ** -0.5, 0.1875, ((1, 4),)),
        "forget_w": bell_draw(arg_keys[9], (D, D_HG), D ** -0.5, 0.1875, ((1, 4),)),
        "input_w": bell_draw(arg_keys[10], (D, D_HG), D ** -0.5, 0.1875, ((1, 4),)),
        "gate_w": bell_draw(arg_keys[11], (D, D_HG), D ** -0.5, 0.1875, ((1, 4),)),
        "memory_rate": jnp.clip(jnp.exp(math.log(32.0) - 4.158883 * jax.random.uniform(arg_keys[12], (D_HG,), jnp.float32) ** shard_levels(arg_keys[12], (D_HG,), ((0, 4),), -0.2, 0.2)), 0.5, 32.0),
        "head_gain": jnp.clip(1.0 + 0.1 * jax.random.normal(arg_keys[13], (D_HG,), jnp.float32), 0.5, 1.5),
        "conv_out_w": bell_draw(arg_keys[14], (D_CONV, D), (2 * D_CONV) ** -0.5, 0.1875, ((0, 4),)),
        "rec_out_w": bell_draw(arg_keys[15], (D_HG, D), (2 * D_HG) ** -0.5, 0.125, ((0, 4),)),
    }


EPS = 1e-06

def reference(frames, norm_gain, conv_value_w, conv_gate_w, conv_taps, conv_bias, channel_gain, channel_shift, query_w, forget_w, input_w, gate_w, memory_rate, head_gain, conv_out_w, rec_out_w):
    values = frames.astype(jnp.float32)
    normed = (values * lax.rsqrt(lax.optimization_barrier(jnp.mean(values * values, axis=-1, keepdims=True)) + EPS) * norm_gain).astype(jnp.bfloat16)
    flat_rows = normed.reshape(SEQS * SEQ_LEN, D)

    def project(weight):
        product = jnp.dot(flat_rows, weight, preferred_element_type=jnp.float32)
        return product.astype(jnp.bfloat16).reshape(SEQS, SEQ_LEN, weight.shape[1])
    conv_value = project(conv_value_w)
    conv_gate = project(conv_gate_w)
    queries = project(query_w)
    forget_raw = project(forget_w)
    inputs = project(input_w)
    out_gate = project(gate_w)
    gated_conv = (conv_value.astype(jnp.float32) * jax.nn.sigmoid(conv_gate.astype(jnp.float32))).astype(jnp.bfloat16)
    filtered = lax.conv_general_dilated(gated_conv, conv_taps[:, None, :], window_strides=(1,), padding=[(CONV_WIDTH - 1, 0)], dimension_numbers=('NWC', 'WIO', 'NWC'), feature_group_count=D_CONV, preferred_element_type=jnp.float32) + conv_bias
    row_mean = lax.optimization_barrier(jnp.mean(filtered, axis=-1, keepdims=True))
    row_var = lax.optimization_barrier(jnp.mean(filtered * filtered, axis=-1, keepdims=True)) - row_mean * row_mean
    scaled = (filtered - row_mean) * lax.rsqrt(row_var + EPS) * channel_gain + channel_shift
    conv_out = jax.nn.silu(scaled).astype(jnp.bfloat16)
    head_shape = (SEQS, SEQ_LEN, HEADS, HEAD)
    rate_rows = (memory_rate / SEQ_LEN).reshape(HEADS, HEAD)
    in_gate = rate_rows * jax.nn.sigmoid(-forget_raw.astype(jnp.float32)).reshape(head_shape)
    log_forget = jnp.log1p(-in_gate)
    query_rows = queries.astype(jnp.float32).reshape(head_shape)
    value_rows = inputs.reshape(head_shape).astype(jnp.float32)

    def to_blocks(array):
        return array.reshape(SEQS, N_SP, POS_DEV, HEADS, HEAD).transpose(1, 0, 2, 3, 4)
    causal = jnp.tril(jnp.ones((POS_DEV, POS_DEV), dtype=bool))
    highest = lax.Precision.HIGHEST

    def advance(carry_state, block_inputs):
        block_query, block_gate, block_forget, block_value = block_inputs
        cumulative = jnp.cumsum(block_forget, axis=1)
        final_sum = cumulative[:, -1]
        grown = (block_query * jnp.exp(cumulative)).astype(jnp.bfloat16).astype(jnp.float32)
        shrunk = (block_gate * jnp.exp(-cumulative)).astype(jnp.bfloat16).astype(jnp.float32)
        weighted = (block_gate * jnp.exp(final_sum[:, None] - cumulative)).astype(jnp.bfloat16).astype(jnp.float32)
        scores = jnp.einsum('sthk,suhk->shtu', grown, shrunk, precision=highest)
        scores = jnp.where(causal, scores, 0.0).astype(jnp.bfloat16).astype(jnp.float32)
        carried_low = carry_state.astype(jnp.bfloat16).astype(jnp.float32)
        block_out = jnp.einsum('shtu,suhv->sthv', scores, block_value, precision=highest)
        block_out = block_out + jnp.einsum('sthk,shkv->sthv', grown, carried_low, precision=highest)
        new_state = jnp.exp(final_sum)[..., None] * carry_state + jnp.einsum('suhk,suhv->shkv', weighted, block_value, precision=highest)
        return (new_state, block_out)
    start_state = jnp.zeros((SEQS, HEADS, HEAD, HEAD), jnp.float32)
    blocks = (to_blocks(query_rows), to_blocks(in_gate), to_blocks(log_forget), to_blocks(value_rows))
    final_state, block_outs = lax.scan(advance, start_state, blocks)
    rec_raw = block_outs.transpose(1, 0, 2, 3, 4).reshape(head_shape)
    rec_norm = rec_raw * lax.rsqrt(lax.optimization_barrier(jnp.mean(rec_raw * rec_raw, axis=-1, keepdims=True)) + EPS) * head_gain.reshape(HEADS, HEAD)
    rec_out = (rec_norm.reshape(SEQS, SEQ_LEN, D_HG) * jax.nn.silu(out_gate.astype(jnp.float32))).astype(jnp.bfloat16)
    conv_part = jnp.dot(conv_out.reshape(SEQS * SEQ_LEN, D_CONV), conv_out_w, preferred_element_type=jnp.float32)
    rec_part = jnp.dot(rec_out.reshape(SEQS * SEQ_LEN, D_HG), rec_out_w, preferred_element_type=jnp.float32)
    return (conv_part + rec_part).astype(jnp.bfloat16).reshape(SEQS, SEQ_LEN, D)
```

```python
import functools

import jax
import jax.numpy as jnp
from jax import lax
from jax.experimental import pallas as pl
from jax.experimental.pallas import tpu as pltpu
from jax.sharding import PartitionSpec as P

HEAD = 128
LANES = 128
EDGE = 32
EPS = 1e-06
MESH = pl.DeviceIdType.MESH
F32 = jnp.float32
BF16 = jnp.bfloat16


def flip(index, mask):
    out, bit = index, 1
    while bit <= mask:
        if mask & bit:
            out = out + bit - 2 * bit * ((index // bit) % 2)
        bit *= 2
    return out


def mm(a, b, dims):
    return lax.dot_general(a, b, (dims, ((), ())), preferred_element_type=F32)


def kernel(
    cfg,
    frames, norm_gain, cvw, cgw, taps, conv_bias, channel_gain, channel_shift,
    qw, fw, iw, gw, rate, head_gain, cow, row,
    out,
    gath, wbuf, ow, norm_v, taps_v, cb_v, cg_v, cs_v, rate_v, hg_v,
    gated, edges, ext, filt, stat, stat_in, conv_send, conv_in, rec_send, rec_in,
    grown_s, shrunk_s, value_s, gate_s, local_s, state, state_in, decay, decay_in, carry_out, carry_in, acc,
    loc_sem, fr_send, fr_recv, ow_send, ow_recv, ed_send, ed_recv, stt_send, stt_recv, dc_send, dc_recv,
    ca_send, ca_recv, sm_send, sm_recv, cv_send, cv_recv, rc_send, rc_recv,
):
    n_tp, n_sp, spt, d_conv, seq_total = cfg
    positions, depth = frames.shape[1], frames.shape[2]
    seqs = n_tp * spt
    conv_n, rec_n = cvw.shape[1], qw.shape[1]
    heads = rec_n // HEAD
    chunk = carry_out.shape[1]
    tp, sp = lax.axis_index("tp"), lax.axis_index("sp")

    barrier = pltpu.get_barrier_semaphore()
    for k in range(1, n_tp):
        pl.semaphore_signal(barrier, inc=1, device_id={"tp": flip(tp, k)}, device_id_type=MESH)
    for d in range(1, n_sp):
        pl.semaphore_signal(barrier, inc=1, device_id={"sp": (sp + d) % n_sp}, device_id_type=MESH)

    offsets = [0, conv_n, 2 * conv_n, 2 * conv_n + rec_n, 2 * conv_n + 2 * rec_n, 2 * conv_n + 3 * rec_n]
    copies = [pltpu.make_async_copy(frames, gath.at[0], loc_sem.at[0])]
    copies.append(pltpu.make_async_copy(norm_gain, norm_v, loc_sem.at[1]))
    for n, (ref, at) in enumerate(zip((cvw, cgw, qw, fw, iw, gw), offsets)):
        copies.append(
            pltpu.make_async_copy(ref, wbuf.at[:, pl.ds(at, ref.shape[1])], loc_sem.at[2 + n])
        )
    small = ((taps, taps_v), (conv_bias, cb_v), (channel_gain, cg_v), (channel_shift, cs_v), (rate, rate_v), (head_gain, hg_v))
    for n, (ref, to) in enumerate(small):
        copies.append(pltpu.make_async_copy(ref, to, loc_sem.at[8 + n]))
    copies.append(pltpu.make_async_copy(cow, ow.at[0, pl.ds(0, conv_n)], loc_sem.at[14]))
    copies.append(pltpu.make_async_copy(row, ow.at[0, pl.ds(conv_n, rec_n)], loc_sem.at[15]))
    for copy in copies:
        copy.start()

    def remote(src, dst, send, recv, **device):
        return pltpu.make_async_remote_copy(
            src_ref=src, dst_ref=dst, send_sem=send, recv_sem=recv, device_id=device, device_id_type=MESH
        )

    direct = [k for k in range(1, n_tp) if k % 2 == 0] + [1]
    fr = [None] * n_tp
    for k in range(1, n_tp):
        if k in direct:
            fr[k] = remote(frames, gath.at[k], fr_send.at[k], fr_recv.at[k], tp=flip(tp, k))
        else:
            fr[k] = remote(gath.at[k - 1], gath.at[k], fr_send.at[k], fr_recv.at[k], tp=flip(tp, 1))
    wt = [None] * n_tp
    for k in range(1, n_tp):
        source, to = (0, k) if k in direct else (k - 1, 1)
        wt[k] = remote(ow.at[source], ow.at[k], ow_send.at[k], ow_recv.at[k], tp=flip(tp, to))

    pl.semaphore_wait(barrier, n_tp - 1 + n_sp - 1)
    for k in direct:
        fr[k].start()
    for copy in copies:
        copy.wait()

    t_row = lax.broadcasted_iota(jnp.int32, (positions, positions), 0)
    t_col = lax.broadcasted_iota(jnp.int32, (positions, positions), 1)
    causal = t_col <= t_row
    lower = jnp.where(causal, 1.0, 0.0).astype(BF16)
    lower3 = jnp.concatenate([lower, lower, lower], axis=1)
    rate_row = rate_v[...] / seq_total

    sent_states = []

    def state_copies(p):
        pair = p * chunk // HEAD
        return (
            remote(state.at[pl.ds(p * chunk, chunk)], state_in.at[sp], stt_send.at[p], stt_recv.at[sp], sp=p),
            remote(decay.at[pair], decay_in.at[sp], dc_send.at[p], dc_recv.at[sp], sp=p),
        )

    def edge_copy(q):
        return remote(
            gated.at[q, pl.ds(positions - EDGE, EDGE)], edges.at[q], ed_send.at[q], ed_recv.at[q], sp=(sp + 1) % n_sp
        )

    for k in range(n_tp):
        if k > 0:
            fr[k].wait_recv()
            if k % 2 == 0:
                fr[k + 1].start()
        if k == min(2, n_tp - 1):
            for j in direct:
                wt[j].start()
        for i in range(spt):
            q = k * spt + i
            x = gath[k, i].astype(F32)
            mean = jnp.mean(x * x, axis=-1, keepdims=True)
            normed = (x * lax.rsqrt(mean + EPS) * norm_v[...]).astype(BF16)

            def project(at, width):
                return mm(normed, wbuf[:, at : at + width], ((1,), (0,))).astype(BF16)

            conv_both = project(0, 2 * conv_n).astype(F32)
            gated_q = (conv_both[:, :conv_n] * jax.nn.sigmoid(conv_both[:, conv_n:])).astype(BF16)
            gated[q] = gated_q
            ext[q, EDGE : EDGE + positions] = gated_q.astype(F32)
            edge_copy(q).start()

            forget_raw = project(offsets[3], rec_n).astype(F32)
            in_gate = rate_row * jax.nn.sigmoid(-forget_raw)
            log_forget = jnp.log1p(-in_gate)
            hi = log_forget.astype(BF16)
            rest = log_forget - hi.astype(F32)
            mid = rest.astype(BF16)
            low = (rest - mid.astype(F32)).astype(BF16)
            cumulative = mm(lower3, jnp.concatenate([hi, mid, low], axis=0), ((1,), (0,)))
            last = cumulative[positions - 1 : positions, :]
            weighted = (in_gate * jnp.exp(last - cumulative)).astype(BF16)
            value = project(offsets[4], rec_n)
            value_s[q] = value
            last_decay = jnp.exp(last)
            for h in range(heads):
                pair = q * heads + h
                lanes = slice(h * HEAD, (h + 1) * HEAD)
                state[pair * HEAD : (pair + 1) * HEAD] = mm(value[:, lanes], weighted[:, lanes], ((0,), (0,)))
                decay[pair] = jnp.broadcast_to(last_decay[:, lanes], (8, HEAD))
                for p in range(pair * HEAD // chunk, (pair + 1) * HEAD // chunk):

                    @pl.when(jnp.logical_and(sp != p, sp < n_sp - 1))
                    def _():
                        for copy in state_copies(p):
                            copy.start()

            shrunk_s[q] = (in_gate * jnp.exp(-cumulative)).astype(BF16)
            queries = project(offsets[2], rec_n).astype(F32)
            grown_s[q] = (queries * jnp.exp(cumulative)).astype(BF16)
            gate_s[q] = project(offsets[5], rec_n)

    reach = taps.shape[0] - 1
    for q in range(seqs):
        edge_copy(q).wait_recv()
        ext[q, 0:EDGE] = jnp.where(sp > 0, edges[q].astype(F32), 0.0)
        total = jnp.broadcast_to(cb_v[...], (positions, conv_n))
        tap_rows = taps_v[...].astype(F32)
        for j in range(reach + 1):
            start = EDGE - reach + j
            total = total + tap_rows[j : j + 1, :] * ext[q, start : start + positions, :]
        filt[q] = total
        lane = lax.broadcasted_iota(jnp.int32, (positions, LANES), 1)
        sums = jnp.sum(total, axis=-1, keepdims=True)
        squares = jnp.sum(total * total, axis=-1, keepdims=True)
        table = jnp.where(lane == 0, sums, jnp.where(lane == 1, squares, 0.0))
        stat[q] = jnp.transpose(table)[0:8, :]

    def stat_copy(k):
        return remote(stat, stat_in.at[k], sm_send.at[k], sm_recv.at[k], tp=flip(tp, k))

    for k in range(1, n_tp):
        stat_copy(k).start()

    own = pl.multiple_of(sp * chunk, chunk)
    state_in[sp] = state[pl.ds(own, chunk), :]
    decay_in[sp] = decay[sp * chunk // HEAD]

    def carry_copy(j):
        return remote(carry_out.at[j], carry_in.at[pl.ds(own, chunk)], ca_send.at[j], ca_recv.at[sp], sp=j)

    def from_source(j):
        return (
            remote(state.at[pl.ds(0, chunk)], state_in.at[j], stt_send.at[j], stt_recv.at[j], sp=j),
            remote(decay.at[0], decay_in.at[j], dc_send.at[j], dc_recv.at[j], sp=j),
        )

    carried = jnp.zeros((chunk, HEAD), F32)
    for j in range(n_sp):
        carry_out[j] = carried.astype(BF16)
        if j > 0:

            @pl.when(sp != j)
            def _():
                carry_copy(j).start()

        if j < n_sp - 1:

            @pl.when(sp != j)
            def _():
                for copy in from_source(j):
                    copy.wait_recv()

            carried = decay_in[j, 0:1, :] * carried + state_in[j]
    carry_in[pl.ds(own, chunk), :] = carry_out[sp]

    for q in range(seqs):
        for h in range(heads):
            lanes = slice(h * HEAD, (h + 1) * HEAD)
            scores = mm(grown_s[q, :, lanes], shrunk_s[q, :, lanes], ((1,), (1,)))
            scores = jnp.where(causal, scores, 0.0).astype(BF16)
            local_s[q, :, lanes] = mm(scores, value_s[q, :, lanes], ((1,), (0,)))

    for k in range(1, n_tp):
        stat_copy(k).wait_recv()

    def conv_copy(k):
        return remote(conv_send.at[k], conv_in.at[k], cv_send.at[k], cv_recv.at[k], tp=flip(tp, k))

    def rec_copy(k):
        return remote(rec_send.at[k], rec_in.at[k], rc_send.at[k], rc_recv.at[k], tp=flip(tp, k))

    order = list(range(n_tp - 1, -1, -1))
    for k in order:
        for i in range(spt):
            q = k * spt + i
            both = stat[q]
            for d in range(1, n_tp):
                both = both + stat_in[d, (k ^ d) * spt + i]
            both = both / d_conv
            table = jnp.concatenate([both, jnp.zeros((LANES - 8, positions), F32)], axis=0)
            table = jnp.transpose(table)
            row_mean = table[:, 0:1]
            row_var = table[:, 1:2] - row_mean * row_mean
            scaled = (filt[q] - row_mean) * lax.rsqrt(row_var + EPS) * cg_v[...] + cs_v[...]
            result = (scaled * jax.nn.sigmoid(scaled)).astype(BF16)
            rows = slice(i * positions, (i + 1) * positions)
            if k == 0:
                conv_in[0, rows] = result
            else:
                conv_send[k, rows] = result
        if k > 0:
            conv_copy(k).start()

    for j in range(n_sp):

        @pl.when(jnp.logical_and(sp != j, sp > 0))
        def _():
            remote(
                carry_out.at[0], carry_in.at[pl.ds(j * chunk, chunk)], ca_send.at[j], ca_recv.at[j], sp=j
            ).wait_recv()

    @pl.when(sp == 0)
    def _():
        carry_in[...] = jnp.zeros_like(carry_in)

    for k in order:
        for i in range(spt):
            q = k * spt + i
            rows = slice(i * positions, (i + 1) * positions)
            for h in range(heads):
                pair = q * heads + h
                lanes = slice(h * HEAD, (h + 1) * HEAD)
                rec_raw = local_s[q, :, lanes] + mm(
                    grown_s[q, :, lanes], carry_in[pair * HEAD : (pair + 1) * HEAD, :], ((1,), (1,))
                )
                mean = jnp.mean(rec_raw * rec_raw, axis=-1, keepdims=True)
                rec_norm = rec_raw * lax.rsqrt(mean + EPS) * hg_v[:, lanes]
                gate = gate_s[q, :, lanes].astype(F32)
                result = (rec_norm * (gate * jax.nn.sigmoid(gate))).astype(BF16)
                if k == 0:
                    rec_in[0, rows, lanes] = result
                else:
                    rec_send[k, rows, lanes] = result
        if k > 0:
            rec_copy(k).start()

    for k in range(2, n_tp, 2):
        wt[k].wait_recv()
        wt[k + 1].start()
    if n_tp > 1:
        wt[1].wait_recv()
    for n, k in enumerate(range(n_tp)):
        if k > 0:
            if k % 2 == 1 and k > 1:
                wt[k].wait_recv()
            conv_copy(k).wait_recv()
            rec_copy(k).wait_recv()
        part = mm(conv_in[k], ow[k, 0:conv_n, :], ((1,), (0,))) + mm(
            rec_in[k], ow[k, conv_n : conv_n + rec_n, :], ((1,), (0,))
        )
        if k == 0:
            acc[...] = part
        elif k < n_tp - 1:
            acc[...] += part
        else:
            out[...] = (acc[...] + part).astype(BF16).reshape(out.shape)

    for k in range(1, n_tp):
        fr[k].wait_send()
        wt[k].wait_send()
        stat_copy(k).wait_send()
        conv_copy(k).wait_send()
        rec_copy(k).wait_send()
    for q in range(seqs):
        edge_copy(q).wait_send()
    for p in range(n_sp):

        @pl.when(jnp.logical_and(sp != p, sp < n_sp - 1))
        def _():
            for copy in state_copies(p):
                copy.wait_send()

        if p > 0:

            @pl.when(sp != p)
            def _():
                carry_copy(p).wait_send()


def wide(array, axis):
    extra = -array.shape[axis] % LANES
    if extra == 0:
        return array
    pads = [(0, 0)] * array.ndim
    pads[axis] = (0, extra)
    return jnp.pad(array, pads)


def local(
    n_tp, n_sp, frames, norm_gain, conv_value_w, conv_gate_w, conv_taps, conv_bias, channel_gain, channel_shift,
    query_w, forget_w, input_w, gate_w, memory_rate, head_gain, conv_out_w, rec_out_w,
):
    d_conv = conv_value_w.shape[1] * n_tp
    spt, positions, depth = frames.shape
    conv_value_w, conv_gate_w, conv_taps = (wide(a, 1) for a in (conv_value_w, conv_gate_w, conv_taps))
    conv_bias, channel_gain, channel_shift, conv_out_w = (
        wide(a, 0) for a in (conv_bias, channel_gain, channel_shift, conv_out_w)
    )
    conv_n, rec_n = conv_value_w.shape[1], query_w.shape[1]
    out_n = rec_out_w.shape[1]
    seqs = n_tp * spt
    heads = rec_n // HEAD
    pairs = seqs * heads
    chunk = pairs * HEAD // n_sp
    width = conv_n * 2 + rec_n * 4
    rows = spt * positions
    vm = pltpu.VMEM
    sem = pltpu.SemaphoreType.DMA
    scratch = [
        vm((n_tp, spt, positions, depth), BF16),
        vm((depth, width), BF16),
        vm((n_tp, conv_n + rec_n, out_n), BF16),
        vm((1, depth), F32),
        vm(conv_taps.shape, BF16),
        vm((1, conv_n), F32),
        vm((1, conv_n), F32),
        vm((1, conv_n), F32),
        vm((1, rec_n), F32),
        vm((1, rec_n), F32),
        vm((seqs, positions, conv_n), BF16),
        vm((seqs, EDGE, conv_n), BF16),
        vm((seqs, EDGE + positions, conv_n), F32),
        vm((seqs, positions, conv_n), F32),
        vm((seqs, 8, positions), F32),
        vm((n_tp, seqs, 8, positions), F32),
        vm((n_tp, rows, conv_n), BF16),
        vm((n_tp, rows, conv_n), BF16),
        vm((n_tp, rows, rec_n), BF16),
        vm((n_tp, rows, rec_n), BF16),
        vm((seqs, positions, rec_n), BF16),
        vm((seqs, positions, rec_n), BF16),
        vm((seqs, positions, rec_n), BF16),
        vm((seqs, positions, rec_n), BF16),
        vm((seqs, positions, rec_n), F32),
        vm((pairs * HEAD, HEAD), F32),
        vm((n_sp, chunk, HEAD), F32),
        vm((pairs, 8, HEAD), F32),
        vm((n_sp, 8, HEAD), F32),
        vm((n_sp, chunk, HEAD), BF16),
        vm((pairs * HEAD, HEAD), BF16),
        vm((rows, out_n), F32),
        sem((16,)),
        sem((n_tp,)), sem((n_tp,)),
        sem((n_tp,)), sem((n_tp,)),
        sem((seqs,)), sem((seqs,)),
        sem((n_sp,)), sem((n_sp,)),
        sem((n_sp,)), sem((n_sp,)),
        sem((n_sp,)), sem((n_sp,)),
        sem((n_tp,)), sem((n_tp,)),
        sem((n_tp,)), sem((n_tp,)),
        sem((n_tp,)), sem((n_tp,)),
    ]
    return pl.pallas_call(
        functools.partial(kernel, (n_tp, n_sp, spt, d_conv, positions * n_sp)),
        out_shape=jax.ShapeDtypeStruct((spt, positions, out_n), BF16),
        in_specs=[pl.BlockSpec(memory_space=pl.ANY)] * 16,
        out_specs=pl.BlockSpec(memory_space=pltpu.VMEM),
        scratch_shapes=scratch,
        compiler_params=pltpu.CompilerParams(
            collective_id=0, has_side_effects=True, vmem_limit_bytes=48 * 1024 * 1024
        ),
    )(
        frames, norm_gain[None], conv_value_w, conv_gate_w, conv_taps, conv_bias[None], channel_gain[None],
        channel_shift[None], query_w, forget_w, input_w, gate_w, memory_rate[None], head_gain[None],
        conv_out_w, rec_out_w,
    )


def solution(mesh):
    placed = (
        P("tp", "sp", None),
        P(),
        P(None, "tp"),
        P(None, "tp"),
        P(None, "tp"),
        P("tp"),
        P("tp"),
        P("tp"),
        P(None, "tp"),
        P(None, "tp"),
        P(None, "tp"),
        P(None, "tp"),
        P("tp"),
        P("tp"),
        P("tp", None),
        P("tp", None),
    )
    return jax.shard_map(
        functools.partial(local, mesh.shape["tp"], mesh.shape["sp"]),
        mesh=mesh, in_specs=placed, out_specs=P("tp", "sp", None), check_vma=False,
    )
```

```python
import functools

import jax
import jax.numpy as jnp
from jax import lax
from jax.experimental import pallas as pl
from jax.experimental.pallas import tpu as pltpu
from jax.sharding import PartitionSpec as P

HEAD = 128
LANES = 128
EDGE = 32
EPS = 1e-06
MESH = pl.DeviceIdType.MESH
F32 = jnp.float32
BF16 = jnp.bfloat16


def flip(index, mask):
    out, bit = index, 1
    while bit <= mask:
        if mask & bit:
            out = out + bit - 2 * bit * ((index // bit) % 2)
        bit *= 2
    return out


def mm(a, b, dims):
    return lax.dot_general(a, b, (dims, ((), ())), preferred_element_type=F32)


def kernel(
    cfg,
    frames, norm_gain, cvw, cgw, taps, conv_bias, channel_gain, channel_shift,
    qw, fw, iw, gw, rate, head_gain, cow, row,
    out,
    gath, wbuf, ow, norm_v, taps_v, cb_v, cg_v, cs_v, rate_v, hg_v,
    gated, edges, ext, filt, stat, stat_in, conv_send, conv_in, rec_send, rec_in,
    grown_s, shrunk_s, value_s, gate_s, local_s, state, state_in, carry_out, carry_in, acc,
    loc_sem, fr_send, fr_recv, ow_send, ow_recv, ed_send, ed_recv, stt_send, stt_recv,
    ca_send, ca_recv, sm_send, sm_recv, cv_send, cv_recv, rc_send, rc_recv,
):
    n_tp, n_sp, spt, d_conv, seq_total = cfg
    positions, depth = frames.shape[1], frames.shape[2]
    seqs = n_tp * spt
    conv_n, rec_n = cvw.shape[1], qw.shape[1]
    heads = rec_n // HEAD
    chunk = carry_out.shape[1]
    groups = carry_out.shape[0] // n_sp
    together = seqs // groups
    tp, sp = lax.axis_index("tp"), lax.axis_index("sp")

    barrier = pltpu.get_barrier_semaphore()
    for k in range(1, n_tp):
        pl.semaphore_signal(barrier, inc=1, device_id={"tp": flip(tp, k)}, device_id_type=MESH)
    for d in range(1, n_sp):
        pl.semaphore_signal(barrier, inc=1, device_id={"sp": (sp + d) % n_sp}, device_id_type=MESH)

    offsets = [0, conv_n, 2 * conv_n, 2 * conv_n + rec_n, 2 * conv_n + 2 * rec_n, 2 * conv_n + 3 * rec_n]
    copies = [pltpu.make_async_copy(frames, gath.at[0], loc_sem.at[0])]
    copies.append(pltpu.make_async_copy(norm_gain, norm_v, loc_sem.at[1]))
    for n, (ref, at) in enumerate(zip((cvw, cgw, qw, fw, iw, gw), offsets)):
        copies.append(
            pltpu.make_async_copy(ref, wbuf.at[:, pl.ds(at, ref.shape[1])], loc_sem.at[2 + n])
        )
    small = ((taps, taps_v), (conv_bias, cb_v), (channel_gain, cg_v), (channel_shift, cs_v), (rate, rate_v), (head_gain, hg_v))
    for n, (ref, to) in enumerate(small):
        copies.append(pltpu.make_async_copy(ref, to, loc_sem.at[8 + n]))
    copies.append(pltpu.make_async_copy(cow, ow.at[0, pl.ds(0, conv_n)], loc_sem.at[14]))
    copies.append(pltpu.make_async_copy(row, ow.at[0, pl.ds(conv_n, rec_n)], loc_sem.at[15]))
    for copy in copies:
        copy.start()

    def remote(src, dst, send, recv, **device):
        return pltpu.make_async_remote_copy(
            src_ref=src, dst_ref=dst, send_sem=send, recv_sem=recv, device_id=device, device_id_type=MESH
        )

    direct = [k for k in range(1, n_tp) if k % 2 == 0] + [1]
    fr = [None] * n_tp
    for k in range(1, n_tp):
        if k in direct:
            fr[k] = remote(frames, gath.at[k], fr_send.at[k], fr_recv.at[k], tp=flip(tp, k))
        else:
            fr[k] = remote(gath.at[k - 1], gath.at[k], fr_send.at[k], fr_recv.at[k], tp=flip(tp, 1))
    wt = [None] * n_tp
    for k in range(1, n_tp):
        source, to = (0, k) if k in direct else (k - 1, 1)
        wt[k] = remote(ow.at[source], ow.at[k], ow_send.at[k], ow_recv.at[k], tp=flip(tp, to))

    pl.semaphore_wait(barrier, n_tp - 1 + n_sp - 1)
    for k in direct:
        fr[k].start()
    for copy in copies[14:]:
        copy.wait()
    for k in direct:
        wt[k].start()
    for copy in copies[:14]:
        copy.wait()

    t_row = lax.broadcasted_iota(jnp.int32, (positions, positions), 0)
    t_col = lax.broadcasted_iota(jnp.int32, (positions, positions), 1)
    causal = t_col <= t_row
    lower = jnp.where(causal, 1.0, 0.0).astype(BF16)
    lower3 = jnp.concatenate([lower, lower, lower], axis=1)
    rate_row = rate_v[...] / seq_total

    def state_copy(g, p):
        n = g * n_sp + p
        return remote(state.at[n], state_in.at[g * n_sp + sp], stt_send.at[n], stt_recv.at[g * n_sp + sp], sp=p)

    def state_from(g, j):
        n = g * n_sp + j
        return remote(state.at[n], state_in.at[n], stt_send.at[n], stt_recv.at[n], sp=j)

    def carry_copy(g, j):
        n = g * n_sp + j
        here = pl.multiple_of((g * n_sp + sp) * chunk, chunk)
        return remote(carry_out.at[n], carry_in.at[pl.ds(here, chunk)], ca_send.at[n], ca_recv.at[g * n_sp + sp], sp=j)

    def carry_from(g, j):
        n = g * n_sp + j
        return remote(carry_out.at[n], carry_in.at[pl.ds(n * chunk, chunk)], ca_send.at[n], ca_recv.at[n], sp=j)

    def scan(g):
        mine = g * n_sp + sp
        state_in[mine] = state[mine]
        carried = jnp.zeros((chunk, HEAD), F32)
        for j in range(n_sp):
            n = g * n_sp + j
            carry_out[n] = carried.astype(BF16)
            if j > 0:

                @pl.when(sp != j)
                def _():
                    carry_copy(g, j).start()

            if j < n_sp - 1:

                @pl.when(sp != j)
                def _():
                    state_from(g, j).wait_recv()

                carried = state_in[n, chunk : chunk + 1, :] * carried + state_in[n, 0:chunk, :]
        here = pl.multiple_of(mine * chunk, chunk)
        carry_in[pl.ds(here, chunk), :] = carry_out[mine]

    def edge_copy(q):
        return remote(
            gated.at[q, pl.ds(positions - EDGE, EDGE)], edges.at[q], ed_send.at[q], ed_recv.at[q], sp=(sp + 1) % n_sp
        )

    for k in range(n_tp):
        if k > 0:
            fr[k].wait_recv()
            if k % 2 == 0:
                fr[k + 1].start()
        for i in range(spt):
            q = k * spt + i
            x = gath[k, i].astype(F32)
            mean = jnp.mean(x * x, axis=-1, keepdims=True)
            normed = (x * lax.rsqrt(mean + EPS) * norm_v[...]).astype(BF16)

            def project(at, width):
                return mm(normed, wbuf[:, at : at + width], ((1,), (0,))).astype(BF16)

            conv_both = project(0, 2 * conv_n).astype(F32)
            gated_q = (conv_both[:, :conv_n] * jax.nn.sigmoid(conv_both[:, conv_n:])).astype(BF16)
            gated[q] = gated_q
            ext[q, EDGE : EDGE + positions] = gated_q.astype(F32)
            edge_copy(q).start()

            forget_raw = project(offsets[3], rec_n).astype(F32)
            in_gate = rate_row * jax.nn.sigmoid(-forget_raw)
            log_forget = jnp.log1p(-in_gate)
            hi = log_forget.astype(BF16)
            rest = log_forget - hi.astype(F32)
            mid = rest.astype(BF16)
            low = (rest - mid.astype(F32)).astype(BF16)
            cumulative = mm(lower3, jnp.concatenate([hi, mid, low], axis=0), ((1,), (0,)))
            last = cumulative[positions - 1 : positions, :]
            weighted = (in_gate * jnp.exp(last - cumulative)).astype(BF16)
            value = project(offsets[4], rec_n)
            value_s[q] = value
            last_decay = jnp.exp(last)
            for h in range(heads):
                pair = q * heads + h
                lanes = slice(h * HEAD, (h + 1) * HEAD)
                block = mm(value[:, lanes], weighted[:, lanes], ((0,), (0,)))
                rows_decay = jnp.broadcast_to(last_decay[:, lanes], (8, HEAD))
                for r in range(HEAD // chunk):
                    n = pair * (HEAD // chunk) + r
                    state[n, 0:chunk] = block[r * chunk : (r + 1) * chunk]
                    state[n, chunk : chunk + 8] = rows_decay
            if (q + 1) % together == 0:
                g = q // together
                for p in range(n_sp):

                    @pl.when(jnp.logical_and(sp != p, sp < n_sp - 1))
                    def _():
                        state_copy(g, p).start()

            shrunk_s[q] = (in_gate * jnp.exp(-cumulative)).astype(BF16)
            queries = project(offsets[2], rec_n).astype(F32)
            grown_s[q] = (queries * jnp.exp(cumulative)).astype(BF16)
            gate_s[q] = project(offsets[5], rec_n)
            if (q + 1) % together == 0 and q // together > 0:
                scan(q // together - 1)

    reach = taps.shape[0] - 1
    for q in range(seqs):
        edge_copy(q).wait_recv()
        ext[q, 0:EDGE] = jnp.where(sp > 0, edges[q].astype(F32), 0.0)
        total = jnp.broadcast_to(cb_v[...], (positions, conv_n))
        tap_rows = taps_v[...].astype(F32)
        for j in range(reach + 1):
            start = EDGE - reach + j
            total = total + tap_rows[j : j + 1, :] * ext[q, start : start + positions, :]
        filt[q] = total
        lane = lax.broadcasted_iota(jnp.int32, (positions, LANES), 1)
        sums = jnp.sum(total, axis=-1, keepdims=True)
        squares = jnp.sum(total * total, axis=-1, keepdims=True)
        table = jnp.where(lane == 0, sums, jnp.where(lane == 1, squares, 0.0))
        stat[q] = jnp.transpose(table)[0:8, :]

    def stat_copy(k):
        return remote(stat, stat_in.at[k], sm_send.at[k], sm_recv.at[k], tp=flip(tp, k))

    for k in range(1, n_tp):
        stat_copy(k).start()

    scan(groups - 1)

    for q in range(seqs):
        for h in range(heads):
            lanes = slice(h * HEAD, (h + 1) * HEAD)
            scores = mm(grown_s[q, :, lanes], shrunk_s[q, :, lanes], ((1,), (1,)))
            scores = jnp.where(causal, scores, 0.0).astype(BF16)
            local_s[q, :, lanes] = mm(scores, value_s[q, :, lanes], ((1,), (0,)))

    for k in range(1, n_tp):
        stat_copy(k).wait_recv()

    def conv_copy(k):
        return remote(conv_send.at[k], conv_in.at[k], cv_send.at[k], cv_recv.at[k], tp=flip(tp, k))

    def rec_copy(k):
        return remote(rec_send.at[k], rec_in.at[k], rc_send.at[k], rc_recv.at[k], tp=flip(tp, k))

    order = list(range(n_tp - 1, -1, -1))
    for k in order:
        for i in range(spt):
            q = k * spt + i
            both = stat[q]
            for d in range(1, n_tp):
                both = both + stat_in[d, (k ^ d) * spt + i]
            both = both / d_conv
            table = jnp.concatenate([both, jnp.zeros((LANES - 8, positions), F32)], axis=0)
            table = jnp.transpose(table)
            row_mean = table[:, 0:1]
            row_var = table[:, 1:2] - row_mean * row_mean
            scaled = (filt[q] - row_mean) * lax.rsqrt(row_var + EPS) * cg_v[...] + cs_v[...]
            result = (scaled * jax.nn.sigmoid(scaled)).astype(BF16)
            rows = slice(i * positions, (i + 1) * positions)
            if k == 0:
                conv_in[0, rows] = result
            else:
                conv_send[k, rows] = result
        if k > 0:
            conv_copy(k).start()

    @pl.when(sp == 0)
    def _():
        carry_in[...] = jnp.zeros_like(carry_in)

    arrived = set()
    for k in [1, 0] + list(range(2, n_tp)):
        for i in range(spt):
            q = k * spt + i
            rows = slice(i * positions, (i + 1) * positions)
            g = q // together
            for j in range(n_sp if g not in arrived else 0):

                @pl.when(jnp.logical_and(sp != j, sp > 0))
                def _():
                    carry_from(g, j).wait_recv()

            arrived.add(g)
            for h in range(heads):
                pair = q * heads + h
                lanes = slice(h * HEAD, (h + 1) * HEAD)
                rec_raw = local_s[q, :, lanes] + mm(
                    grown_s[q, :, lanes], carry_in[pair * HEAD : (pair + 1) * HEAD, :], ((1,), (1,))
                )
                mean = jnp.mean(rec_raw * rec_raw, axis=-1, keepdims=True)
                rec_norm = rec_raw * lax.rsqrt(mean + EPS) * hg_v[:, lanes]
                gate = gate_s[q, :, lanes].astype(F32)
                result = (rec_norm * (gate * jax.nn.sigmoid(gate))).astype(BF16)
                if k == 0:
                    rec_in[0, rows, lanes] = result
                else:
                    rec_send[k, rows, lanes] = result
        if k > 0:
            rec_copy(k).start()

    for k in range(2, n_tp, 2):
        wt[k].wait_recv()
        wt[k + 1].start()
    if n_tp > 1:
        wt[1].wait_recv()
    for n, k in enumerate(range(n_tp)):
        if k > 0:
            if k % 2 == 1 and k > 1:
                wt[k].wait_recv()
            conv_copy(k).wait_recv()
            rec_copy(k).wait_recv()
        part = mm(conv_in[k], ow[k, 0:conv_n, :], ((1,), (0,))) + mm(
            rec_in[k], ow[k, conv_n : conv_n + rec_n, :], ((1,), (0,))
        )
        if k == 0:
            acc[...] = part
        elif k < n_tp - 1:
            acc[...] += part
        else:
            out[...] = (acc[...] + part).astype(BF16).reshape(out.shape)

    for k in range(1, n_tp):
        fr[k].wait_send()
        wt[k].wait_send()
        stat_copy(k).wait_send()
        conv_copy(k).wait_send()
        rec_copy(k).wait_send()
    for q in range(seqs):
        edge_copy(q).wait_send()
    for g in range(groups):
        for p in range(n_sp):

            @pl.when(jnp.logical_and(sp != p, sp < n_sp - 1))
            def _():
                state_copy(g, p).wait_send()

            if p > 0:

                @pl.when(sp != p)
                def _():
                    carry_copy(g, p).wait_send()


def wide(array, axis):
    extra = -array.shape[axis] % LANES
    if extra == 0:
        return array
    pads = [(0, 0)] * array.ndim
    pads[axis] = (0, extra)
    return jnp.pad(array, pads)


def local(
    n_tp, n_sp, frames, norm_gain, conv_value_w, conv_gate_w, conv_taps, conv_bias, channel_gain, channel_shift,
    query_w, forget_w, input_w, gate_w, memory_rate, head_gain, conv_out_w, rec_out_w,
):
    d_conv = conv_value_w.shape[1] * n_tp
    spt, positions, depth = frames.shape
    conv_value_w, conv_gate_w, conv_taps = (wide(a, 1) for a in (conv_value_w, conv_gate_w, conv_taps))
    conv_bias, channel_gain, channel_shift, conv_out_w = (
        wide(a, 0) for a in (conv_bias, channel_gain, channel_shift, conv_out_w)
    )
    conv_n, rec_n = conv_value_w.shape[1], query_w.shape[1]
    out_n = rec_out_w.shape[1]
    seqs = n_tp * spt
    heads = rec_n // HEAD
    pairs = seqs * heads
    together = 1
    while together < seqs and together * heads * HEAD // n_sp < 16:
        together *= 2
    groups = seqs // together
    chunk = together * heads * HEAD // n_sp
    slots = groups * n_sp
    width = conv_n * 2 + rec_n * 4
    rows = spt * positions
    vm = pltpu.VMEM
    sem = pltpu.SemaphoreType.DMA
    scratch = [
        vm((n_tp, spt, positions, depth), BF16),
        vm((depth, width), BF16),
        vm((n_tp, conv_n + rec_n, out_n), BF16),
        vm((1, depth), F32),
        vm(conv_taps.shape, BF16),
        vm((1, conv_n), F32),
        vm((1, conv_n), F32),
        vm((1, conv_n), F32),
        vm((1, rec_n), F32),
        vm((1, rec_n), F32),
        vm((seqs, positions, conv_n), BF16),
        vm((seqs, EDGE, conv_n), BF16),
        vm((seqs, EDGE + positions, conv_n), F32),
        vm((seqs, positions, conv_n), F32),
        vm((seqs, 8, positions), F32),
        vm((n_tp, seqs, 8, positions), F32),
        vm((n_tp, rows, conv_n), BF16),
        vm((n_tp, rows, conv_n), BF16),
        vm((n_tp, rows, rec_n), BF16),
        vm((n_tp, rows, rec_n), BF16),
        vm((seqs, positions, rec_n), BF16),
        vm((seqs, positions, rec_n), BF16),
        vm((seqs, positions, rec_n), BF16),
        vm((seqs, positions, rec_n), BF16),
        vm((seqs, positions, rec_n), F32),
        vm((slots, chunk + 8, HEAD), F32),
        vm((slots, chunk + 8, HEAD), F32),
        vm((slots, chunk, HEAD), BF16),
        vm((pairs * HEAD, HEAD), BF16),
        vm((rows, out_n), F32),
        sem((16,)),
        sem((n_tp,)), sem((n_tp,)),
        sem((n_tp,)), sem((n_tp,)),
        sem((seqs,)), sem((seqs,)),
        sem((slots,)), sem((slots,)),
        sem((slots,)), sem((slots,)),
        sem((n_tp,)), sem((n_tp,)),
        sem((n_tp,)), sem((n_tp,)),
        sem((n_tp,)), sem((n_tp,)),
    ]
    return pl.pallas_call(
        functools.partial(kernel, (n_tp, n_sp, spt, d_conv, positions * n_sp)),
        out_shape=jax.ShapeDtypeStruct((spt, positions, out_n), BF16),
        in_specs=[pl.BlockSpec(memory_space=pltpu.HBM)] * 16,
        out_specs=pl.BlockSpec(memory_space=pltpu.VMEM),
        scratch_shapes=scratch,
        compiler_params=pltpu.CompilerParams(
            collective_id=0, has_side_effects=True, vmem_limit_bytes=56 * 1024 * 1024
        ),
    )(
        frames, norm_gain[None], conv_value_w, conv_gate_w, conv_taps, conv_bias[None], channel_gain[None],
        channel_shift[None], query_w, forget_w, input_w, gate_w, memory_rate[None], head_gain[None],
        conv_out_w, rec_out_w,
    )


def solution(mesh):
    placed = (
        P("tp", "sp", None),
        P(),
        P(None, "tp"),
        P(None, "tp"),
        P(None, "tp"),
        P("tp"),
        P("tp"),
        P("tp"),
        P(None, "tp"),
        P(None, "tp"),
        P(None, "tp"),
        P(None, "tp"),
        P("tp"),
        P("tp"),
        P("tp", None),
        P("tp", None),
    )
    return jax.shard_map(
        functools.partial(local, mesh.shape["tp"], mesh.shape["sp"]),
        mesh=mesh, in_specs=placed, out_specs=P("tp", "sp", None), check_vma=False,
    )
```

```python
import functools

import jax
import jax.numpy as jnp
from jax import lax
from jax.experimental import pallas as pl
from jax.experimental.pallas import tpu as pltpu
from jax.sharding import PartitionSpec as P

HEAD = 128
LANES = 128
EDGE = 32
EPS = 1e-06
MESH = pl.DeviceIdType.MESH
F32 = jnp.float32
BF16 = jnp.bfloat16


def flip(index, mask):
    out, bit = index, 1
    while bit <= mask:
        if mask & bit:
            out = out + bit - 2 * bit * ((index // bit) % 2)
        bit *= 2
    return out


def mm(a, b, dims):
    return lax.dot_general(a, b, (dims, ((), ())), preferred_element_type=F32)


def kernel(
    cfg,
    frames, norm_gain, cvw, cgw, taps, conv_bias, channel_gain, channel_shift,
    qw, fw, iw, gw, rate, head_gain, cow, row,
    out,
    gath, wbuf, ow, norm_v, taps_v, cb_v, cg_v, cs_v, rate_v, hg_v,
    gated, edges, ext, filt, stat, stat_in, conv_send, conv_in, rec_send, rec_in,
    grown_s, shrunk_s, value_s, gate_s, local_s, state, state_in, carry_out, carry_in, acc,
    loc_sem, fr_send, fr_recv, ow_send, ow_recv, ed_send, ed_recv, stt_send, stt_recv,
    ca_send, ca_recv, sm_send, sm_recv, cv_send, cv_recv, rc_send, rc_recv, wc_send, wc_recv,
):
    n_tp, n_sp, spt, d_conv, seq_total = cfg
    positions, depth = frames.shape[1], frames.shape[2]
    seqs = n_tp * spt
    conv_n, rec_n = cvw.shape[1], qw.shape[1]
    heads = rec_n // HEAD
    chunk = carry_out.shape[1]
    groups = carry_out.shape[0] // n_sp
    together = seqs // groups
    tp, sp = lax.axis_index("tp"), lax.axis_index("sp")

    barrier = pltpu.get_barrier_semaphore()
    for k in range(1, n_tp):
        pl.semaphore_signal(barrier, inc=1, device_id={"tp": flip(tp, k)}, device_id_type=MESH)
    for d in range(1, n_sp):
        pl.semaphore_signal(barrier, inc=1, device_id={"sp": (sp + d) % n_sp}, device_id_type=MESH)

    offsets = [0, conv_n, 2 * conv_n, 2 * conv_n + rec_n, 2 * conv_n + 2 * rec_n, 2 * conv_n + 3 * rec_n]
    copies = [pltpu.make_async_copy(frames, gath.at[0], loc_sem.at[0])]
    copies.append(pltpu.make_async_copy(norm_gain, norm_v, loc_sem.at[1]))
    for n, (ref, at) in enumerate(zip((cvw, cgw, qw, fw, iw, gw), offsets)):
        copies.append(
            pltpu.make_async_copy(ref, wbuf.at[:, pl.ds(at, ref.shape[1])], loc_sem.at[2 + n])
        )
    small = ((taps, taps_v), (conv_bias, cb_v), (channel_gain, cg_v), (channel_shift, cs_v), (rate, rate_v), (head_gain, hg_v))
    for n, (ref, to) in enumerate(small):
        copies.append(pltpu.make_async_copy(ref, to, loc_sem.at[8 + n]))
    copies.append(pltpu.make_async_copy(cow, ow.at[0, pl.ds(0, conv_n)], loc_sem.at[14]))
    copies.append(pltpu.make_async_copy(row, ow.at[0, pl.ds(conv_n, rec_n)], loc_sem.at[15]))
    for copy in copies:
        copy.start()

    def remote(src, dst, send, recv, **device):
        return pltpu.make_async_remote_copy(
            src_ref=src, dst_ref=dst, send_sem=send, recv_sem=recv, device_id=device, device_id_type=MESH
        )

    direct = [k for k in range(1, n_tp) if k % 2 == 0] + [1]
    fr = [None] * n_tp
    for k in range(1, n_tp):
        if k in direct:
            fr[k] = remote(frames, gath.at[k], fr_send.at[k], fr_recv.at[k], tp=flip(tp, k))
        else:
            fr[k] = remote(gath.at[k - 1], gath.at[k], fr_send.at[k], fr_recv.at[k], tp=flip(tp, 1))
    wt = [None] * n_tp
    for k in range(1, n_tp):
        source, to = (0, k) if k in direct else (k - 1, 1)
        wt[k] = remote(ow.at[source], ow.at[k], ow_send.at[k], ow_recv.at[k], tp=flip(tp, to))

    wc = {}
    for k in range(2, n_tp, 2):
        late, early = pl.ds(0, conv_n), pl.ds(conv_n, rec_n)
        wt[k] = remote(ow.at[0, early], ow.at[k, early], ow_send.at[k], ow_recv.at[k], tp=flip(tp, k))
        wc[k] = remote(ow.at[0, late], ow.at[k, late], wc_send.at[k], wc_recv.at[k], tp=flip(tp, k))

    pl.semaphore_wait(barrier, n_tp - 1 + n_sp - 1)
    for k in direct:
        fr[k].start()
    for copy in copies[14:]:
        copy.wait()
    for k in direct:
        wt[k].start()
    for copy in copies[:14]:
        copy.wait()

    t_row = lax.broadcasted_iota(jnp.int32, (positions, positions), 0)
    t_col = lax.broadcasted_iota(jnp.int32, (positions, positions), 1)
    causal = t_col <= t_row
    lower = jnp.where(causal, 1.0, 0.0).astype(BF16)
    lower3 = jnp.concatenate([lower, lower, lower], axis=1)
    rate_row = rate_v[...] / seq_total

    def state_copy(g, p):
        n = g * n_sp + p
        return remote(state.at[n], state_in.at[g * n_sp + sp], stt_send.at[n], stt_recv.at[g * n_sp + sp], sp=p)

    def state_from(g, j):
        n = g * n_sp + j
        return remote(state.at[n], state_in.at[n], stt_send.at[n], stt_recv.at[n], sp=j)

    def carry_copy(g, j):
        n = g * n_sp + j
        here = pl.multiple_of((g * n_sp + sp) * chunk, chunk)
        return remote(carry_out.at[n], carry_in.at[pl.ds(here, chunk)], ca_send.at[n], ca_recv.at[g * n_sp + sp], sp=j)

    def carry_from(g, j):
        n = g * n_sp + j
        return remote(carry_out.at[n], carry_in.at[pl.ds(n * chunk, chunk)], ca_send.at[n], ca_recv.at[n], sp=j)

    def scan(g):
        mine = g * n_sp + sp
        state_in[mine] = state[mine]
        carried = jnp.zeros((chunk, HEAD), F32)
        for j in range(n_sp):
            n = g * n_sp + j
            carry_out[n] = carried.astype(BF16)
            if j > 0:

                @pl.when(sp != j)
                def _():
                    carry_copy(g, j).start()

            if j < n_sp - 1:

                @pl.when(sp != j)
                def _():
                    state_from(g, j).wait_recv()

                carried = state_in[n, chunk : chunk + 1, :] * carried + state_in[n, 0:chunk, :]
        here = pl.multiple_of(mine * chunk, chunk)
        carry_in[pl.ds(here, chunk), :] = carry_out[mine]

    def edge_copy(q):
        return remote(
            gated.at[q, pl.ds(positions - EDGE, EDGE)], edges.at[q], ed_send.at[q], ed_recv.at[q], sp=(sp + 1) % n_sp
        )

    for k in range(n_tp):
        if k > 0:
            fr[k].wait_recv()
            if k % 2 == 0:
                fr[k + 1].start()
        for i in range(spt):
            q = k * spt + i
            x = gath[k, i].astype(F32)
            mean = jnp.mean(x * x, axis=-1, keepdims=True)
            normed = (x * lax.rsqrt(mean + EPS) * norm_v[...]).astype(BF16)

            def project(at, width):
                return mm(normed, wbuf[:, at : at + width], ((1,), (0,))).astype(BF16)

            conv_both = project(0, 2 * conv_n).astype(F32)
            gated_q = (conv_both[:, :conv_n] * jax.nn.sigmoid(conv_both[:, conv_n:])).astype(BF16)
            gated[q] = gated_q
            ext[q, EDGE : EDGE + positions] = gated_q.astype(F32)
            edge_copy(q).start()

            forget_raw = project(offsets[3], rec_n).astype(F32)
            in_gate = rate_row * jax.nn.sigmoid(-forget_raw)
            log_forget = jnp.log1p(-in_gate)
            hi = log_forget.astype(BF16)
            rest = log_forget - hi.astype(F32)
            mid = rest.astype(BF16)
            low = (rest - mid.astype(F32)).astype(BF16)
            cumulative = mm(lower3, jnp.concatenate([hi, mid, low], axis=0), ((1,), (0,)))
            last = cumulative[positions - 1 : positions, :]
            weighted = (in_gate * jnp.exp(last - cumulative)).astype(BF16)
            value = project(offsets[4], rec_n)
            value_s[q] = value
            last_decay = jnp.exp(last)
            for h in range(heads):
                pair = q * heads + h
                lanes = slice(h * HEAD, (h + 1) * HEAD)
                block = mm(value[:, lanes], weighted[:, lanes], ((0,), (0,)))
                rows_decay = jnp.broadcast_to(last_decay[:, lanes], (8, HEAD))
                for r in range(HEAD // chunk):
                    n = pair * (HEAD // chunk) + r
                    state[n, 0:chunk] = block[r * chunk : (r + 1) * chunk]
                    state[n, chunk : chunk + 8] = rows_decay
            if (q + 1) % together == 0:
                g = q // together
                for p in range(n_sp):

                    @pl.when(jnp.logical_and(sp != p, sp < n_sp - 1))
                    def _():
                        state_copy(g, p).start()

            shrunk_s[q] = (in_gate * jnp.exp(-cumulative)).astype(BF16)
            queries = project(offsets[2], rec_n).astype(F32)
            grown_s[q] = (queries * jnp.exp(cumulative)).astype(BF16)
            gate_s[q] = project(offsets[5], rec_n)
            if (q + 1) % together == 0 and q // together > 0:
                scan(q // together - 1)

    reach = taps.shape[0] - 1
    for q in range(seqs):
        edge_copy(q).wait_recv()
        ext[q, 0:EDGE] = jnp.where(sp > 0, edges[q].astype(F32), 0.0)
        total = jnp.broadcast_to(cb_v[...], (positions, conv_n))
        tap_rows = taps_v[...].astype(F32)
        for j in range(reach + 1):
            start = EDGE - reach + j
            total = total + tap_rows[j : j + 1, :] * ext[q, start : start + positions, :]
        filt[q] = total
        lane = lax.broadcasted_iota(jnp.int32, (positions, LANES), 1)
        sums = jnp.sum(total, axis=-1, keepdims=True)
        squares = jnp.sum(total * total, axis=-1, keepdims=True)
        table = jnp.where(lane == 0, sums, jnp.where(lane == 1, squares, 0.0))
        stat[q] = jnp.transpose(table)[0:8, :]

    def stat_copy(k):
        return remote(stat, stat_in.at[k], sm_send.at[k], sm_recv.at[k], tp=flip(tp, k))

    for k in range(1, n_tp):
        stat_copy(k).start()
    for k in wc:
        wc[k].start()

    scan(groups - 1)

    for q in range(seqs):
        for h in range(heads):
            lanes = slice(h * HEAD, (h + 1) * HEAD)
            scores = mm(grown_s[q, :, lanes], shrunk_s[q, :, lanes], ((1,), (1,)))
            scores = jnp.where(causal, scores, 0.0).astype(BF16)
            local_s[q, :, lanes] = mm(scores, value_s[q, :, lanes], ((1,), (0,)))

    for k in range(1, n_tp):
        stat_copy(k).wait_recv()

    def conv_copy(k):
        return remote(conv_send.at[k], conv_in.at[k], cv_send.at[k], cv_recv.at[k], tp=flip(tp, k))

    def rec_copy(k):
        return remote(rec_send.at[k], rec_in.at[k], rc_send.at[k], rc_recv.at[k], tp=flip(tp, k))

    order = list(range(n_tp - 1, -1, -1))
    for k in order:
        for i in range(spt):
            q = k * spt + i
            both = stat[q]
            for d in range(1, n_tp):
                both = both + stat_in[d, (k ^ d) * spt + i]
            both = both / d_conv
            table = jnp.concatenate([both, jnp.zeros((LANES - 8, positions), F32)], axis=0)
            table = jnp.transpose(table)
            row_mean = table[:, 0:1]
            row_var = table[:, 1:2] - row_mean * row_mean
            scaled = (filt[q] - row_mean) * lax.rsqrt(row_var + EPS) * cg_v[...] + cs_v[...]
            result = (scaled * jax.nn.sigmoid(scaled)).astype(BF16)
            rows = slice(i * positions, (i + 1) * positions)
            if k == 0:
                conv_in[0, rows] = result
            else:
                conv_send[k, rows] = result
        if k > 0:
            conv_copy(k).start()

    @pl.when(sp == 0)
    def _():
        carry_in[...] = jnp.zeros_like(carry_in)

    arrived = set()
    for k in [1, 0] + list(range(2, n_tp)):
        for i in range(spt):
            q = k * spt + i
            rows = slice(i * positions, (i + 1) * positions)
            g = q // together
            for j in range(n_sp if g not in arrived else 0):

                @pl.when(jnp.logical_and(sp != j, sp > 0))
                def _():
                    carry_from(g, j).wait_recv()

            arrived.add(g)
            for h in range(heads):
                pair = q * heads + h
                lanes = slice(h * HEAD, (h + 1) * HEAD)
                rec_raw = local_s[q, :, lanes] + mm(
                    grown_s[q, :, lanes], carry_in[pair * HEAD : (pair + 1) * HEAD, :], ((1,), (1,))
                )
                mean = jnp.mean(rec_raw * rec_raw, axis=-1, keepdims=True)
                rec_norm = rec_raw * lax.rsqrt(mean + EPS) * hg_v[:, lanes]
                gate = gate_s[q, :, lanes].astype(F32)
                result = (rec_norm * (gate * jax.nn.sigmoid(gate))).astype(BF16)
                if k == 0:
                    rec_in[0, rows, lanes] = result
                else:
                    rec_send[k, rows, lanes] = result
        if k > 0:
            rec_copy(k).start()

    for k in range(2, n_tp, 2):
        wt[k].wait_recv()
        wc[k].wait_recv()
        wt[k + 1].start()
    if n_tp > 1:
        wt[1].wait_recv()
    for n, k in enumerate(range(n_tp)):
        if k > 0:
            if k % 2 == 1 and k > 1:
                wt[k].wait_recv()
            conv_copy(k).wait_recv()
            rec_copy(k).wait_recv()
        part = mm(conv_in[k], ow[k, 0:conv_n, :], ((1,), (0,))) + mm(
            rec_in[k], ow[k, conv_n : conv_n + rec_n, :], ((1,), (0,))
        )
        if k == 0:
            acc[...] = part
        elif k < n_tp - 1:
            acc[...] += part
        else:
            out[...] = (acc[...] + part).astype(BF16).reshape(out.shape)

    for k in range(1, n_tp):
        fr[k].wait_send()
        wt[k].wait_send()
        if k in wc:
            wc[k].wait_send()
        stat_copy(k).wait_send()
        conv_copy(k).wait_send()
        rec_copy(k).wait_send()
    for q in range(seqs):
        edge_copy(q).wait_send()
    for g in range(groups):
        for p in range(n_sp):

            @pl.when(jnp.logical_and(sp != p, sp < n_sp - 1))
            def _():
                state_copy(g, p).wait_send()

            if p > 0:

                @pl.when(sp != p)
                def _():
                    carry_copy(g, p).wait_send()


def wide(array, axis):
    extra = -array.shape[axis] % LANES
    if extra == 0:
        return array
    pads = [(0, 0)] * array.ndim
    pads[axis] = (0, extra)
    return jnp.pad(array, pads)


def local(
    n_tp, n_sp, frames, norm_gain, conv_value_w, conv_gate_w, conv_taps, conv_bias, channel_gain, channel_shift,
    query_w, forget_w, input_w, gate_w, memory_rate, head_gain, conv_out_w, rec_out_w,
):
    d_conv = conv_value_w.shape[1] * n_tp
    spt, positions, depth = frames.shape
    conv_value_w, conv_gate_w, conv_taps = (wide(a, 1) for a in (conv_value_w, conv_gate_w, conv_taps))
    conv_bias, channel_gain, channel_shift, conv_out_w = (
        wide(a, 0) for a in (conv_bias, channel_gain, channel_shift, conv_out_w)
    )
    conv_n, rec_n = conv_value_w.shape[1], query_w.shape[1]
    out_n = rec_out_w.shape[1]
    seqs = n_tp * spt
    heads = rec_n // HEAD
    pairs = seqs * heads
    together = 1
    while together < seqs and together * heads * HEAD // n_sp < 16:
        together *= 2
    groups = seqs // together
    chunk = together * heads * HEAD // n_sp
    slots = groups * n_sp
    width = conv_n * 2 + rec_n * 4
    rows = spt * positions
    vm = pltpu.VMEM
    sem = pltpu.SemaphoreType.DMA
    scratch = [
        vm((n_tp, spt, positions, depth), BF16),
        vm((depth, width), BF16),
        vm((n_tp, conv_n + rec_n, out_n), BF16),
        vm((1, depth), F32),
        vm(conv_taps.shape, BF16),
        vm((1, conv_n), F32),
        vm((1, conv_n), F32),
        vm((1, conv_n), F32),
        vm((1, rec_n), F32),
        vm((1, rec_n), F32),
        vm((seqs, positions, conv_n), BF16),
        vm((seqs, EDGE, conv_n), BF16),
        vm((seqs, EDGE + positions, conv_n), F32),
        vm((seqs, positions, conv_n), F32),
        vm((seqs, 8, positions), F32),
        vm((n_tp, seqs, 8, positions), F32),
        vm((n_tp, rows, conv_n), BF16),
        vm((n_tp, rows, conv_n), BF16),
        vm((n_tp, rows, rec_n), BF16),
        vm((n_tp, rows, rec_n), BF16),
        vm((seqs, positions, rec_n), BF16),
        vm((seqs, positions, rec_n), BF16),
        vm((seqs, positions, rec_n), BF16),
        vm((seqs, positions, rec_n), BF16),
        vm((seqs, positions, rec_n), F32),
        vm((slots, chunk + 8, HEAD), F32),
        vm((slots, chunk + 8, HEAD), F32),
        vm((slots, chunk, HEAD), BF16),
        vm((pairs * HEAD, HEAD), BF16),
        vm((rows, out_n), F32),
        sem((16,)),
        sem((n_tp,)), sem((n_tp,)),
        sem((n_tp,)), sem((n_tp,)),
        sem((seqs,)), sem((seqs,)),
        sem((slots,)), sem((slots,)),
        sem((slots,)), sem((slots,)),
        sem((n_tp,)), sem((n_tp,)),
        sem((n_tp,)), sem((n_tp,)),
        sem((n_tp,)), sem((n_tp,)),
        sem((n_tp,)), sem((n_tp,)),
    ]
    return pl.pallas_call(
        functools.partial(kernel, (n_tp, n_sp, spt, d_conv, positions * n_sp)),
        out_shape=jax.ShapeDtypeStruct((spt, positions, out_n), BF16),
        in_specs=[pl.BlockSpec(memory_space=pltpu.HBM)] * 16,
        out_specs=pl.BlockSpec(memory_space=pltpu.VMEM),
        scratch_shapes=scratch,
        compiler_params=pltpu.CompilerParams(
            collective_id=0, has_side_effects=True, vmem_limit_bytes=56 * 1024 * 1024
        ),
    )(
        frames, norm_gain[None], conv_value_w, conv_gate_w, conv_taps, conv_bias[None], channel_gain[None],
        channel_shift[None], query_w, forget_w, input_w, gate_w, memory_rate[None], head_gain[None],
        conv_out_w, rec_out_w,
    )


def solution(mesh):
    placed = (
        P("tp", "sp", None),
        P(),
        P(None, "tp"),
        P(None, "tp"),
        P(None, "tp"),
        P("tp"),
        P("tp"),
        P("tp"),
        P(None, "tp"),
        P(None, "tp"),
        P(None, "tp"),
        P(None, "tp"),
        P("tp"),
        P("tp"),
        P("tp", None),
        P("tp", None),
    )
    return jax.shard_map(
        functools.partial(local, mesh.shape["tp"], mesh.shape["sp"]),
        mesh=mesh, in_specs=placed, out_specs=P("tp", "sp", None), check_vma=False,
    )
```
